32 devices in a mesh: ep: 8 (over z, y), tp: 4 (over x, core).
Axes of the slice: x: 2, y: 2, z: 4, core: 2. Of those that a mesh axis runs over, the one named last changes fastest.
Arguments:
- resid: bfloat16 [256, 2048], P('ep'), may hold values from -6 to 6
- mix_gain: bfloat16 [2048], replicated, may hold values from 0.099609375 to 1.8984375
- proj_x: bfloat16 [2048, 512], P(None, 'tp'), may hold values from -0.125 to 0.125
- proj_z: bfloat16 [2048, 512], P(None, 'tp'), may hold values from -0.125 to 0.125
- proj_b: bfloat16 [2048, 512], P(None, 'tp'), may hold values from -0.125 to 0.125
- proj_c: bfloat16 [2048, 512], P(None, 'tp'), may hold values from -0.125 to 0.125
- proj_step: bfloat16 [2048, 8], replicated, may hold values from -0.125 to 0.125
- step_bias: float32 [8], P('tp'), may hold values from -5 to -1
- decay_rate: float32 [8], P('tp'), may hold values from 1 to 16
- conv_taps: bfloat16 [3, 4, 512], P(None, None, 'tp'), may hold values from -3 to 3
- conv_state: bfloat16 [256, 3, 3, 512], P('ep', None, None, 'tp'), may hold values from -6 to 6
- scan_state: float32 [256, 8, 64, 128], P('ep', 'tp'), may hold values from -2.5 to 2.5
- inner_gain: bfloat16 [512], P('tp'), may hold values from 0.099609375 to 1.8984375
- proj_out: bfloat16 [512, 2048], P('tp'), may hold values from -0.25 to 0.25
- post_gain: bfloat16 [2048], replicated, may hold values from 0.099609375 to 1.8984375
- ffn_gain: bfloat16 [2048], replicated, may hold values from 0.099609375 to 1.8984375
- group_router: bfloat16 [2048, 2], replicated, may hold values from -0.125 to 0.125
- expert_router: bfloat16 [2048, 8], replicated, may hold values from -0.125 to 0.125
- route_experts: int32 [256, 4], P('ep'), may hold values from 0 to 7, as said below
- expert_gate: bfloat16 [8, 2048, 1024], P('ep', None, 'tp'), may hold values from -0.125 to 0.125
- expert_up: bfloat16 [8, 2048, 1024], P('ep', None, 'tp'), may hold values from -0.125 to 0.125
- expert_down: bfloat16 [8, 1024, 2048], P('ep', 'tp')
- dense_switch: bfloat16 [2048], replicated, may hold values from -0.125 to 0.125
- dense_gate: bfloat16 [2048, 2048], P('ep', 'tp'), may hold values from -0.125 to 0.125
- dense_up: bfloat16 [2048, 2048], P('ep', 'tp'), may hold values from -0.125 to 0.125
- dense_down: bfloat16 [2048, 2048], P('ep', 'tp')
- out_gain: bfloat16 [2048], P('tp'), may hold values from 0.099609375 to 1.8984375
Outputs:
- layer_out: bfloat16 [256, 2048], P('ep', 'tp')
- new_state: float32 [256, 8, 64, 128], P('ep', 'tp')
- new_conv: bfloat16 [256, 3, 3, 512], P('ep', None, None, 'tp')
The draws below stay inside these ranges and needn't reach their ends.
Inputs may be any that keep to these rules, and one draw needn't show every extreme that they name: `route_experts`: each row names 4 different experts, all from one group of 4 consecutive expert numbers. Within each aligned block of 32 rows (the rows of one index of ep) no expert is named more than 32 times, and one expert, the same in every block, is named exactly 32 times in every block.
All inputs are finite; a program needn't handle non-finite values.
Results may differ from the reference program's by a relative error of at most 0.019.
Values may be sent and summed in bfloat16 or wider, within the bound.
A program may use at most 64 MiB of HBM per device.

```python
import math
import jax
import jax.numpy as jnp
from jax import lax

MODEL_WIDTH = 2048
HEAD_COUNT = 8
HEAD_DIM = 64
STATE_DIM = 128
STATE_GROUPS = 4
CONV_TAPS = 4
EXPERT_WIDTH = 1024
DENSE_WIDTH = 2048
ROUTE_GROUPS = 2
ROUTE_PICKS = 4
SEQ_DEV = 32
INNER_WIDTH = 512
EXPERTS = 8
GROUP_EXPERTS = 4
CAPACITY = 32
TOKENS = 256
N_TP = 4


def draw_route_experts(key, part):
    blocks = TOKENS // SEQ_DEV
    hot_key, block_key = jax.random.split(jax.random.fold_in(key, 11))
    hot = jax.random.randint(hot_key, (), 0, EXPERTS)
    hot_group = hot // GROUP_EXPERTS
    hot_local = hot % GROUP_EXPERTS
    needed = (CAPACITY - 1) * GROUP_EXPERTS // ROUTE_PICKS + 1

    def one_block(index):
        keys = jax.random.split(jax.random.fold_in(block_key, index), 5)
        hot_rows = jax.random.randint(keys[0], (), needed, SEQ_DEV + 1)
        other = jax.random.randint(keys[1], (SEQ_DEV,), 0, ROUTE_GROUPS - 1)
        other = other + (other >= hot_group).astype(jnp.int32)
        position = jnp.arange(SEQ_DEV)
        group_of = jnp.where(position < hot_rows, hot_group, other)
        group_of = jax.random.permutation(keys[2], group_of)
        member = (group_of[:, None] == jnp.arange(ROUTE_GROUPS)[None, :]).astype(jnp.int32)
        rank = jnp.sum((jnp.cumsum(member, axis=0) - member) * member, axis=1)
        orders = jax.vmap(lambda inner: jax.random.permutation(inner, GROUP_EXPERTS))(jax.random.split(keys[3], ROUTE_GROUPS))
        offsets = jax.random.randint(keys[4], (ROUTE_GROUPS,), 0, GROUP_EXPERTS)
        hot_place = jnp.argmax((orders[hot_group] == hot_local).astype(jnp.int32))
        offsets = offsets.at[hot_group].set(hot_place)
        order_rows = orders[group_of]
        places = (offsets[group_of][:, None] + rank[:, None] * ROUTE_PICKS + jnp.arange(ROUTE_PICKS)[None, :]) % GROUP_EXPERTS
        local = jnp.take_along_axis(order_rows, places, axis=1)
        return (group_of[:, None] * GROUP_EXPERTS + local).astype(jnp.int32)
    return jax.vmap(one_block)(jnp.arange(blocks)).reshape(TOKENS, ROUTE_PICKS)


def column_ramp(width):
    ramp = jnp.arange(width, dtype=jnp.float32) / width
    return 0.5 * jnp.power(10.0, ramp)


def draw_expert_down(key, part):
    base = jax.random.truncated_normal(jax.random.fold_in(key, 21), -6.0, 6.0, (EXPERTS, EXPERT_WIDTH, MODEL_WIDTH), jnp.float32)
    base = base * EXPERT_WIDTH ** (-0.5)
    return (base * column_ramp(MODEL_WIDTH)[None, None, :]).astype(jnp.bfloat16)


def draw_dense_down(key, part):
    base = jax.random.truncated_normal(jax.random.fold_in(key, 31), -6.0, 6.0, (DENSE_WIDTH, MODEL_WIDTH), jnp.float32)
    base = base * DENSE_WIDTH ** (-0.5)
    return (base * column_ramp(MODEL_WIDTH)[None, :]).astype(jnp.bfloat16)


def shard_levels(own_key, shape, shards, smallest, top_value):
    level, own = 1.0, jax.random.fold_in(own_key, 6)
    for dim, blocks in shards:
        heights = jnp.exp(jax.random.uniform(jax.random.fold_in(own, dim), (blocks,), jnp.float32, smallest / len(shards), top_value / len(shards)))
        level = level * jnp.repeat(heights, shape[dim] // blocks).reshape([-1 if axis == dim else 1 for axis in range(len(shape))])
    return level


def normal_values(stream_key, extent, scale, limit, shards=(), held_as=jnp.bfloat16):
    values = jax.random.normal(stream_key, extent, jnp.float32) * scale
    if len(shards) > 0:
        values = shard_levels(stream_key, extent, shards, -0.22, 0.18) * values
    return jnp.clip(values, min=-limit, max=limit).astype(held_as)


def setup_inputs(seed: int = 0) -> dict:
    key_of = jax.random.split(jax.random.key(seed), 28)
    resid = normal_values(key_of[0], (TOKENS, MODEL_WIDTH), 1.0, 6.0, ((0, 8),))
    mix_gain = jnp.clip(1.0 + 0.18 * jax.random.normal(key_of[1], (MODEL_WIDTH,), jnp.float32), 0.099609375, 1.8984375).astype(jnp.bfloat16)
    proj_x = normal_values(key_of[2], (MODEL_WIDTH, INNER_WIDTH), MODEL_WIDTH ** -0.5, 0.125, ((1, 4),))
    proj_z = normal_values(key_of[3], (MODEL_WIDTH, INNER_WIDTH), MODEL_WIDTH ** -0.5, 0.125, ((1, 4),))
    proj_b = normal_values(key_of[4], (MODEL_WIDTH, STATE_GROUPS * STATE_DIM), MODEL_WIDTH ** -0.5, 0.125, ((1, 4),))
    proj_c = normal_values(key_of[5], (MODEL_WIDTH, STATE_GROUPS * STATE_DIM), MODEL_WIDTH ** -0.5, 0.125, ((1, 4),))
    proj_step = normal_values(key_of[6], (MODEL_WIDTH, HEAD_COUNT), MODEL_WIDTH ** -0.5, 0.125)
    step_bias = jnp.clip(-5.0 + 4.0 * jax.random.uniform(key_of[7], (HEAD_COUNT,), jnp.float32) ** shard_levels(key_of[7], (HEAD_COUNT,), ((0, 4),), -0.2, 0.2), -5.0, -1.0)
    decay_rate = jnp.clip(jnp.exp(math.log(16.0) - 2.7725887 * jax.random.uniform(key_of[8], (HEAD_COUNT,), jnp.float32) ** shard_levels(key_of[8], (HEAD_COUNT,), ((0, 4),), -0.2, 0.2)), 1.0, 16.0)
    conv_taps = normal_values(key_of[9], (3, CONV_TAPS, INNER_WIDTH), CONV_TAPS ** -0.5, 3.0, ((2, 4),))
    conv_state = normal_values(key_of[10], (TOKENS, 3, CONV_TAPS - 1, INNER_WIDTH), 1.0, 6.0, ((0, 8), (3, 4)))
    scan_state = normal_values(key_of[11], (TOKENS, HEAD_COUNT, HEAD_DIM, STATE_DIM), 0.3, 2.5, ((0, 8), (1, 4)), jnp.float32)
    inner_gain = jnp.clip(1.0 + 0.18 * jax.random.normal(key_of[12], (INNER_WIDTH,), jnp.float32), 0.099609375, 1.8984375).astype(jnp.bfloat16)
    proj_out = normal_values(key_of[13], (INNER_WIDTH, MODEL_WIDTH), INNER_WIDTH ** -0.5, 0.25, ((0, 4),))
    post_gain = jnp.clip(1.0 + 0.18 * jax.random.normal(key_of[14], (MODEL_WIDTH,), jnp.float32), 0.099609375, 1.8984375).astype(jnp.bfloat16)
    ffn_gain = jnp.clip(1.0 + 0.18 * jax.random.normal(key_of[15], (MODEL_WIDTH,), jnp.float32), 0.099609375, 1.8984375).astype(jnp.bfloat16)
    group_router = normal_values(key_of[16], (MODEL_WIDTH, ROUTE_GROUPS), MODEL_WIDTH ** -0.5, 0.125)
    expert_router = normal_values(key_of[17], (MODEL_WIDTH, EXPERTS), MODEL_WIDTH ** -0.5, 0.125)
    route_experts = draw_route_experts(jax.random.fold_in(key_of[27], 71), 0)
    expert_gate = normal_values(key_of[19], (EXPERTS, MODEL_WIDTH, EXPERT_WIDTH), MODEL_WIDTH ** -0.5, 0.125, ((0, 8), (2, 4)))
    expert_up = normal_values(key_of[20], (EXPERTS, MODEL_WIDTH, EXPERT_WIDTH), MODEL_WIDTH ** -0.5, 0.125, ((0, 8), (2, 4)))
    expert_down = draw_expert_down(jax.random.fold_in(key_of[27], 71), 0)
    dense_switch = normal_values(key_of[22], (MODEL_WIDTH,), MODEL_WIDTH ** -0.5, 0.125)
    dense_gate = normal_values(key_of[23], (DENSE_WIDTH, MODEL_WIDTH), MODEL_WIDTH ** -0.5, 0.125, ((0, 8), (1, 4)))
    dense_up = normal_values(key_of[24], (DENSE_WIDTH, MODEL_WIDTH), MODEL_WIDTH ** -0.5, 0.125, ((0, 8), (1, 4)))
    dense_down = draw_dense_down(jax.random.fold_in(key_of[27], 71), 0)
    out_gain = jnp.clip(1.0 + 0.18 * jax.random.normal(key_of[26], (MODEL_WIDTH,), jnp.float32), 0.099609375, 1.8984375).astype(jnp.bfloat16)
    return dict(resid=resid, mix_gain=mix_gain, proj_x=proj_x, proj_z=proj_z, proj_b=proj_b, proj_c=proj_c, proj_step=proj_step, step_bias=step_bias, decay_rate=decay_rate, conv_taps=conv_taps, conv_state=conv_state, scan_state=scan_state, inner_gain=inner_gain, proj_out=proj_out, post_gain=post_gain, ffn_gain=ffn_gain, group_router=group_router, expert_router=expert_router, route_experts=route_experts, expert_gate=expert_gate, expert_up=expert_up, expert_down=expert_down, dense_switch=dense_switch, dense_gate=dense_gate, dense_up=dense_up, dense_down=dense_down, out_gain=out_gain)


norm_eps = 1e-06

def scaled_rows(values, gain):
    values = values.astype(jnp.float32)
    mean_square = lax.optimization_barrier(jnp.mean(values * values, axis=-1, keepdims=True))
    return values * lax.rsqrt(mean_square + norm_eps) * gain.astype(jnp.float32)

def softmax_plain(logits):
    weights = jnp.exp(logits)
    return weights / lax.optimization_barrier(jnp.sum(weights, axis=-1, keepdims=True))

def state_block(pieces):
    old_state, keep, driven, b_heads, c_heads = pieces
    updated = keep[:, :, None, None] * old_state + driven[:, :, :, None] * b_heads[:, :, None, :]
    read = lax.optimization_barrier(jnp.sum(updated * c_heads[:, :, None, :], axis=3))
    return (updated, read)

def expert_block(pieces):
    rows, gate_weight, up_weight, down_weight = pieces
    gate_value = jnp.dot(rows, gate_weight, preferred_element_type=jnp.float32)
    up_value = jnp.dot(rows, up_weight, preferred_element_type=jnp.float32)
    hidden = (jax.nn.silu(gate_value) * up_value).astype(jnp.bfloat16)
    share = hidden.shape[1] // N_TP
    parts = jnp.einsum('rqf,qfd->qrd', hidden.reshape(rows.shape[0], N_TP, share).astype(jnp.float32), down_weight.reshape(N_TP, share, down_weight.shape[1]).astype(jnp.float32))
    parts = lax.optimization_barrier(parts.astype(jnp.bfloat16))
    return lax.optimization_barrier(jnp.sum(parts.astype(jnp.float32), axis=0)).astype(jnp.bfloat16)

def reference(resid, mix_gain, proj_x, proj_z, proj_b, proj_c, proj_step, step_bias, decay_rate, conv_taps, conv_state, scan_state, inner_gain, proj_out, post_gain, ffn_gain, group_router, expert_router, route_experts, expert_gate, expert_up, expert_down, dense_switch, dense_gate, dense_up, dense_down, out_gain):
    normed = scaled_rows(resid, mix_gain).astype(jnp.bfloat16)
    fresh = jnp.stack([jnp.dot(normed, proj_x, preferred_element_type=jnp.float32), jnp.dot(normed, proj_b, preferred_element_type=jnp.float32), jnp.dot(normed, proj_c, preferred_element_type=jnp.float32)], axis=1).astype(jnp.bfloat16)
    gate_z = jnp.dot(normed, proj_z, preferred_element_type=jnp.float32)
    step_raw = jnp.dot(normed, proj_step, preferred_element_type=jnp.float32)
    history = jnp.concatenate([conv_state, fresh[:, :, None, :]], axis=2)
    activated = jax.nn.silu(lax.optimization_barrier(jnp.sum(history.astype(jnp.float32) * conv_taps.astype(jnp.float32)[None], axis=2)))
    repeat = HEAD_COUNT // STATE_GROUPS
    xs_heads = activated[:, 0].reshape(TOKENS, HEAD_COUNT, HEAD_DIM)
    b_heads = jnp.repeat(activated[:, 1].reshape(TOKENS, STATE_GROUPS, STATE_DIM), repeat, axis=1)
    c_heads = jnp.repeat(activated[:, 2].reshape(TOKENS, STATE_GROUPS, STATE_DIM), repeat, axis=1)
    step = jax.nn.softplus(step_raw + step_bias)
    keep = jnp.exp(-decay_rate * step)
    driven = step[:, :, None] * xs_heads
    blocks = TOKENS // SEQ_DEV

    def by_block(array):
        return array.reshape((blocks, SEQ_DEV) + array.shape[1:])
    new_state, read = lax.map(state_block, (by_block(scan_state), by_block(keep), by_block(driven), by_block(b_heads), by_block(c_heads)))
    new_state = new_state.reshape(scan_state.shape)
    read = read.reshape(TOKENS, INNER_WIDTH)
    gated = (read * jax.nn.silu(gate_z) * inner_gain.astype(jnp.float32)).astype(jnp.bfloat16)
    mixed = jnp.dot(gated, proj_out, preferred_element_type=jnp.float32)
    stream = (resid.astype(jnp.float32) + scaled_rows(mixed, post_gain)).astype(jnp.bfloat16)
    feed = scaled_rows(stream, ffn_gain).astype(jnp.bfloat16)
    group_prob = softmax_plain(jnp.dot(feed, group_router, preferred_element_type=jnp.float32))
    expert_logits = jnp.dot(feed, expert_router, preferred_element_type=jnp.float32)
    matches = route_experts[:, :, None] == jnp.arange(EXPERTS, dtype=jnp.int32)[None, None, :]
    pick_logits = lax.optimization_barrier(jnp.sum(jnp.where(matches, expert_logits[:, None, :], 0.0), axis=2))
    chosen_group = route_experts[:, 0] // GROUP_EXPERTS
    group_weight = lax.optimization_barrier(jnp.sum(jnp.where(chosen_group[:, None] == jnp.arange(ROUTE_GROUPS, dtype=jnp.int32)[None, :], group_prob, 0.0), axis=1))
    pick_weight = softmax_plain(pick_logits) * group_weight[:, None]
    flat_picks = route_experts.reshape(blocks, SEQ_DEV * ROUTE_PICKS)
    one_hot = (flat_picks[:, :, None] == jnp.arange(EXPERTS, dtype=jnp.int32)[None, None, :]).astype(jnp.int32)
    slot = lax.optimization_barrier(jnp.sum((jnp.cumsum(one_hot, axis=1) - one_hot) * one_hot, axis=2))
    block_ids = jnp.arange(blocks, dtype=jnp.int32)[:, None]
    target = ((flat_picks * blocks + block_ids) * CAPACITY + slot).reshape(-1).astype(jnp.int32)
    repeated = jnp.repeat(feed, ROUTE_PICKS, axis=0)
    buffer = jnp.zeros((EXPERTS * blocks * CAPACITY, MODEL_WIDTH), jnp.bfloat16).at[target].set(repeated)
    served = lax.map(expert_block, (buffer.reshape(EXPERTS, blocks * CAPACITY, MODEL_WIDTH), expert_gate, expert_up, expert_down))
    expert_out = served.reshape(-1, MODEL_WIDTH)[target].reshape(TOKENS, ROUTE_PICKS, MODEL_WIDTH)
    routed = lax.optimization_barrier(jnp.sum(expert_out.astype(jnp.float32) * pick_weight[:, :, None], axis=1))
    dense_pre_gate = jnp.dot(feed, dense_gate.T, preferred_element_type=jnp.float32)
    dense_pre_up = jnp.dot(feed, dense_up.T, preferred_element_type=jnp.float32)
    dense_hidden = (jax.nn.silu(dense_pre_gate) * dense_pre_up).astype(jnp.bfloat16)
    dense_out = jnp.dot(dense_hidden, dense_down, preferred_element_type=jnp.float32)
    switch = jax.nn.sigmoid(jnp.dot(feed, dense_switch, preferred_element_type=jnp.float32))
    combined = routed + switch[:, None] * dense_out
    layer_out = (stream.astype(jnp.float32) + scaled_rows(combined, out_gain)).astype(jnp.bfloat16)
    new_conv = history[:, :, 1:, :]
    return (layer_out, new_state, new_conv)
```

```python
import functools

import jax
import jax.numpy as jnp
from jax import lax
from jax.experimental import pallas as pl
from jax.experimental.pallas import tpu as pltpu
from jax.sharding import PartitionSpec as P

norm_eps = 1e-06


def scaled_rows(values, gain):
    values = values.astype(jnp.float32)
    mean_square = jnp.mean(values * values, axis=-1, keepdims=True)
    return values * lax.rsqrt(mean_square + norm_eps) * gain.astype(jnp.float32)


def softmax_plain(logits):
    weights = jnp.exp(logits)
    return weights / jnp.sum(weights, axis=-1, keepdims=True)


def fused_kernel(
    ep,
    group_size,
    group_count,
    expert_count,
    gated_ref,
    proj_out_ref,
    resid_ref,
    post_ref,
    ffn_ref,
    router_ref,
    route_ref,
    out_gain_ref,
    gate_hbm,
    up_hbm,
    down_hbm,
    dense_gate_hbm,
    dense_up_hbm,
    dense_down_hbm,
    out_ref,
    gate_w,
    up_w,
    down_w,
    dgate,
    dup,
    ddown,
    stream_buf,
    mix_own,
    mix_peer,
    half_own,
    half_far,
    rows_buf,
    aux_buf,
    part_buf,
    part_peer,
    send_x,
    recv_x,
    send_ep,
    recv_ep,
    square_own,
    square_peer,
    local_sem,
    dense_send,
    dense_recv,
    mix_send,
    mix_recv,
    rows_send,
    rows_recv,
    aux_send,
    aux_recv,
    forward_send,
    forward_recv,
    part_send,
    part_recv,
    x_send,
    x_recv,
    ep_send,
    ep_recv,
    square_send,
    square_recv,
):
    f32, bf16 = jnp.float32, jnp.bfloat16
    me = lax.axis_index("ep")
    tp = lax.axis_index("tp")
    far = tp // 2
    core = tp % 2
    beside = far * 2 + (1 - core)
    across = (1 - far) * 2 + core
    diagonal = (1 - far) * 2 + (1 - core)
    near = (beside, across, diagonal)
    seqs, width = resid_ref.shape
    quarter = width // 4
    share = dgate.shape[1]

    def remote(src, dst, send, recv, ep_to, tp_to):
        return pltpu.make_async_remote_copy(
            src_ref=src,
            dst_ref=dst,
            send_sem=send,
            recv_sem=recv,
            device_id=(ep_to, tp_to),
            device_id_type=pl.DeviceIdType.MESH,
        )

    def ep_at(step):
        return lax.rem(me + step + ep, ep)

    local = []

    def load(src, dst):
        copy = pltpu.make_async_copy(src, dst, local_sem.at[len(local)])
        copy.start()
        local.append(copy)

    load(gate_hbm.at[0], gate_w)
    load(up_hbm.at[0], up_w)
    for q in range(4):
        load(down_hbm.at[0, :, pl.ds(q * quarter, quarter)], down_w.at[q])
    dense_pairs = ((dense_gate_hbm, dgate), (dense_up_hbm, dup), (dense_down_hbm, ddown))
    for src, dst in dense_pairs:
        load(src.at[pl.ds(tp * share, share), :], dst.at[tp])

    barrier = pltpu.get_barrier_semaphore()
    for step in range(1, ep):
        pl.semaphore_signal(
            barrier, inc=1, device_id=(ep_at(step), tp), device_id_type=pl.DeviceIdType.MESH
        )
    for peer in near:
        pl.semaphore_signal(
            barrier, inc=1, device_id=(me, peer), device_id_type=pl.DeviceIdType.MESH
        )

    mix_own[...] = jnp.dot(
        gated_ref[...], proj_out_ref[...], preferred_element_type=f32
    ).astype(bf16)
    pl.semaphore_wait(barrier, ep - 1 + 3)

    sends = []
    first = remote(mix_own, mix_peer, mix_send.at[0], mix_recv.at[0], me, beside)
    first.start()
    sends.append(first)
    first.wait_recv()
    half = width // 2
    chip_sum = (mix_own[...].astype(f32) + mix_peer[...].astype(f32)).astype(bf16)
    half_own[0] = chip_sum[:, :half]
    half_own[1] = chip_sum[:, half:]
    halves = []
    for k, peer in enumerate((across, diagonal)):
        copy = remote(
            half_own.at[core],
            half_far.at[core],
            mix_send.at[1 + k],
            mix_recv.at[1 + k],
            me,
            peer,
        )
        copy.start()
        halves.append(copy)
    sends += halves

    dense_copies = []
    for t, (src, dst) in enumerate(dense_pairs):
        for k, peer in enumerate(near):
            copy = remote(
                src.at[pl.ds(peer * share, share), :],
                dst.at[tp],
                dense_send.at[3 * t + k],
                dense_recv.at[3 * t + k],
                me,
                peer,
            )
            copy.start()
            dense_copies.append(copy)
    sends += dense_copies
    for copy in halves:
        copy.wait_recv()

    far_sum = jnp.concatenate([half_far[0], half_far[1]], axis=1)
    mixed = chip_sum.astype(f32) + far_sum.astype(f32)
    mixed_scale = lax.rsqrt(jnp.mean(mixed * mixed, axis=1, keepdims=True) + norm_eps)
    stream = (
        resid_ref[...].astype(f32) + mixed * mixed_scale * post_ref[...].astype(f32)
    ).astype(bf16)
    stream_f = stream.astype(f32)
    feed_scale = lax.rsqrt(jnp.mean(stream_f * stream_f, axis=1, keepdims=True) + norm_eps)
    feed = (stream_f * feed_scale * ffn_ref[...].astype(f32)).astype(bf16)
    for q in range(4):
        rows_buf[q, 0] = feed[:, q * quarter : (q + 1) * quarter]
        stream_buf[q] = stream[:, q * quarter : (q + 1) * quarter]

    rows_copies = []
    for step in range(1, ep):
        copy = remote(
            rows_buf.at[tp, 0],
            rows_buf.at[tp, step],
            rows_send.at[step],
            rows_recv.at[step],
            ep_at(step),
            tp,
        )
        copy.start()
        rows_copies.append(copy)
    sends += rows_copies

    logits = lax.dot_general(
        feed, router_ref[...], (((1,), (1,)), ((), ())), preferred_element_type=f32
    )
    lane = lax.broadcasted_iota(jnp.int32, logits.shape, 1)
    route = route_ref[...]
    picked = lane == route[:, 0:1]
    for k in range(1, route.shape[1]):
        picked = picked | (lane == route[:, k : k + 1])
    weights = jnp.exp(logits)
    pick = jnp.where(picked, weights, 0.0)
    group_lane = (lane - expert_count) * group_size
    in_groups = (lane >= expert_count) & (lane < expert_count + group_count)
    group = jnp.where(in_groups, weights, 0.0)
    lead = route[:, 0:1]
    chosen = in_groups & (lead >= group_lane) & (lead < group_lane + group_size)
    group_weight = jnp.sum(jnp.where(chosen, weights, 0.0), axis=1, keepdims=True) / jnp.sum(
        group, axis=1, keepdims=True
    )
    pick = pick / jnp.sum(pick, axis=1, keepdims=True) * group_weight
    switch_lane = expert_count + group_count
    aux_buf[0] = jnp.where(lane == switch_lane, jax.nn.sigmoid(logits), pick).astype(bf16)
    aux_copies = []
    for step in range(1, ep):
        copy = remote(
            aux_buf.at[0],
            aux_buf.at[step],
            aux_send.at[step],
            aux_recv.at[step],
            ep_at(step),
            tp,
        )
        copy.start()
        aux_copies.append(copy)
    sends += aux_copies

    to_beside, to_across, to_last = [], [], []
    for step in range(1, ep):
        rows_copies[step - 1].wait_recv()
        for k, (peer, kept) in enumerate(((across, to_across), (beside, to_beside))):
            copy = remote(
                rows_buf.at[tp, step],
                rows_buf.at[tp, step],
                forward_send.at[k, step],
                forward_recv.at[k, step],
                me,
                peer,
            )
            copy.start()
            kept.append(copy)
    for step in range(1, ep):
        to_across[step - 1].wait_recv()
        copy = remote(
            rows_buf.at[across, step],
            rows_buf.at[across, step],
            forward_send.at[2, step],
            forward_recv.at[2, step],
            me,
            beside,
        )
        copy.start()
        to_last.append(copy)
    sends += to_across + to_beside + to_last
    for copy in local:
        copy.wait()
    for copy in dense_copies + aux_copies + to_beside + to_last:
        copy.wait_recv()

    total = ep * seqs
    gate = up = dense_g = dense_u = None
    nt = (((1,), (1,)), ((), ()))

    def add(total_sum, value):
        return value if total_sum is None else total_sum + value

    for q in range(4):
        rows = rows_buf[q].reshape(total, quarter)
        span = pl.ds(q * quarter, quarter)
        gate = add(gate, jnp.dot(rows, gate_w[span, :], preferred_element_type=f32))
        up = add(up, jnp.dot(rows, up_w[span, :], preferred_element_type=f32))
        dense_g = add(dense_g, lax.dot_general(rows, dgate[q], nt, preferred_element_type=f32))
        dense_u = add(dense_u, lax.dot_general(rows, dup[q], nt, preferred_element_type=f32))
    aux = aux_buf[...].reshape(total, aux_buf.shape[2]).astype(f32)
    aux_lane = lax.broadcasted_iota(jnp.int32, aux.shape, 1)
    weight = jnp.sum(jnp.where(aux_lane == me, aux, 0.0), axis=1, keepdims=True)
    switch = jnp.sum(jnp.where(aux_lane == switch_lane, aux, 0.0), axis=1, keepdims=True)
    hidden = (gate * jax.nn.sigmoid(gate) * up * weight).astype(bf16)
    dense_hidden = (dense_g * jax.nn.sigmoid(dense_g) * dense_u * switch).astype(bf16)

    part_copies = []
    for k, q in enumerate((diagonal, beside, across, tp)):
        value = jnp.dot(hidden, down_w[q], preferred_element_type=f32) + jnp.dot(
            dense_hidden, ddown[q], preferred_element_type=f32
        )
        part_buf[q] = value.astype(bf16).reshape(ep, seqs, quarter)
        if k < 2:
            copy = remote(
                part_buf.at[q], part_peer.at[k], part_send.at[k], part_recv.at[k], me, beside
            )
            copy.start()
            part_copies.append(copy)
    sends += part_copies

    order = list(range(1, ep)) + [0]
    part_copies[0].wait_recv()
    x_copies = {}
    for step in order:
        send_x[step] = (
            part_buf[across, step].astype(f32) + part_peer[0, step].astype(f32)
        ).astype(bf16)
        copy = remote(
            send_x.at[step], recv_x.at[step], x_send.at[step], x_recv.at[step], me, across
        )
        copy.start()
        x_copies[step] = copy
        sends.append(copy)
    part_copies[1].wait_recv()
    combined = None
    ep_copies = []
    for step in order:
        x_copies[step].wait_recv()
        value = (
            part_buf[tp, step].astype(f32)
            + part_peer[1, step].astype(f32)
            + recv_x[step].astype(f32)
        )
        if step == 0:
            combined = value
            continue
        send_ep[step] = value.astype(bf16)
        copy = remote(
            send_ep.at[step],
            recv_ep.at[step],
            ep_send.at[step],
            ep_recv.at[step],
            ep_at(-step),
            tp,
        )
        copy.start()
        ep_copies.append(copy)
    sends += ep_copies
    for step in range(1, ep):
        ep_copies[step - 1].wait_recv()
        combined = combined + recv_ep[step].astype(f32)

    square = jnp.sum(combined * combined, axis=1, keepdims=True)
    square_own[...] = jnp.broadcast_to(square, square_own.shape)
    square_copies = []
    for k, peer in enumerate(near):
        copy = remote(
            square_own, square_peer.at[k], square_send.at[k], square_recv.at[k], me, peer
        )
        copy.start()
        square_copies.append(copy)
    sends += square_copies
    for copy in square_copies:
        copy.wait_recv()
    everything = (square_own[...] + square_peer[0]) + (square_peer[1] + square_peer[2])
    scale = lax.rsqrt(everything[:, 0:1] / width + norm_eps)
    own_stream = stream_buf[tp].astype(f32)
    out_ref[...] = (own_stream + combined * scale * out_gain_ref[...].astype(f32)).astype(bf16)
    for copy in sends:
        copy.wait_send()


def fused_tail(
    gated,
    proj_out,
    resid,
    post_gain,
    ffn_gain,
    group_router,
    expert_router,
    route_experts,
    expert_gate,
    expert_up,
    expert_down,
    dense_switch,
    dense_gate,
    dense_up,
    dense_down,
    out_gain,
):
    ep = lax.axis_size("ep")
    seqs, width = resid.shape
    quarter = width // 4
    expert_count = expert_router.shape[1]
    group_count = group_router.shape[1]
    used = expert_count + group_count + 1
    lanes = -(-used // 128) * 128
    router = jnp.concatenate(
        [
            expert_router.T,
            group_router.T,
            dense_switch[None, :],
            jnp.zeros((lanes - used, width), expert_router.dtype),
        ],
        axis=0,
    )
    hidden_here = expert_gate.shape[2]
    share = dense_gate.shape[0] // 4
    bf16 = jnp.bfloat16
    vmem = pl.BlockSpec(memory_space=pltpu.VMEM)
    hbm = pl.BlockSpec(memory_space=pl.ANY)
    dma = pltpu.SemaphoreType.DMA
    kernel = functools.partial(
        fused_kernel, ep, expert_count // group_count, group_count, expert_count
    )
    return pl.pallas_call(
        kernel,
        out_shape=jax.ShapeDtypeStruct((seqs, quarter), bf16),
        in_specs=[vmem] * 8 + [hbm] * 6,
        out_specs=vmem,
        scratch_shapes=[
            pltpu.VMEM((width, hidden_here), bf16),
            pltpu.VMEM((width, hidden_here), bf16),
            pltpu.VMEM((4, hidden_here, quarter), bf16),
            pltpu.VMEM((4, share, quarter), bf16),
            pltpu.VMEM((4, share, quarter), bf16),
            pltpu.VMEM((4, share, quarter), bf16),
            pltpu.VMEM((4, seqs, quarter), bf16),
            pltpu.VMEM((seqs, width), bf16),
            pltpu.VMEM((seqs, width), bf16),
            pltpu.VMEM((2, seqs, width // 2), bf16),
            pltpu.VMEM((2, seqs, width // 2), bf16),
            pltpu.VMEM((4, ep, seqs, quarter), bf16),
            pltpu.VMEM((ep, seqs, lanes), bf16),
            pltpu.VMEM((4, ep, seqs, quarter), bf16),
            pltpu.VMEM((2, ep, seqs, quarter), bf16),
            pltpu.VMEM((ep, seqs, quarter), bf16),
            pltpu.VMEM((ep, seqs, quarter), bf16),
            pltpu.VMEM((ep, seqs, quarter), bf16),
            pltpu.VMEM((ep, seqs, quarter), bf16),
            pltpu.VMEM((seqs, 128), jnp.float32),
            pltpu.VMEM((3, seqs, 128), jnp.float32),
            dma((9,)),
            dma((9,)),
            dma((9,)),
            dma((3,)),
            dma((3,)),
            dma((ep,)),
            dma((ep,)),
            dma((ep,)),
            dma((ep,)),
            dma((3, ep)),
            dma((3, ep)),
            dma((2,)),
            dma((2,)),
            dma((ep,)),
            dma((ep,)),
            dma((ep,)),
            dma((ep,)),
            dma((3,)),
            dma((3,)),
        ],
        compiler_params=pltpu.CompilerParams(collective_id=0, has_side_effects=True),
        name="fused_tail",
    )(
        gated,
        proj_out,
        resid,
        post_gain[None, :],
        ffn_gain[None, :],
        router,
        route_experts,
        out_gain[None, :],
        expert_gate,
        expert_up,
        expert_down,
        dense_gate,
        dense_up,
        dense_down,
    )


def on_device(
    resid,
    mix_gain,
    proj_x,
    proj_z,
    proj_b,
    proj_c,
    proj_step,
    step_bias,
    decay_rate,
    conv_taps,
    conv_state,
    scan_state,
    inner_gain,
    proj_out,
    post_gain,
    ffn_gain,
    group_router,
    expert_router,
    route_experts,
    expert_gate,
    expert_up,
    expert_down,
    dense_switch,
    dense_gate,
    dense_up,
    dense_down,
    out_gain,
):
    tp_index = lax.axis_index("tp")
    seqs = resid.shape[0]
    width = resid.shape[1]
    quarter = width // lax.axis_size("tp")
    heads_here = scan_state.shape[1]
    head_dim = scan_state.shape[2]
    state_dim = scan_state.shape[3]
    channels = conv_state.shape[3]
    repeat = heads_here // (channels // state_dim)
    normed = scaled_rows(resid, mix_gain).astype(jnp.bfloat16)
    fresh = jnp.stack(
        [
            jnp.dot(normed, proj_x, preferred_element_type=jnp.float32),
            jnp.dot(normed, proj_b, preferred_element_type=jnp.float32),
            jnp.dot(normed, proj_c, preferred_element_type=jnp.float32),
        ],
        axis=1,
    ).astype(jnp.bfloat16)
    gate_z = jnp.dot(normed, proj_z, preferred_element_type=jnp.float32)
    step_all = jnp.dot(normed, proj_step, preferred_element_type=jnp.float32)
    step_raw = lax.dynamic_slice_in_dim(step_all, tp_index * heads_here, heads_here, 1)
    history = jnp.concatenate([conv_state, fresh[:, :, None, :]], axis=2)
    activated = jax.nn.silu(
        jnp.sum(history.astype(jnp.float32) * conv_taps.astype(jnp.float32)[None], axis=2)
    )
    xs_heads = activated[:, 0].reshape(seqs, heads_here, head_dim)
    b_heads = jnp.repeat(activated[:, 1].reshape(seqs, -1, state_dim), repeat, axis=1)
    c_heads = jnp.repeat(activated[:, 2].reshape(seqs, -1, state_dim), repeat, axis=1)
    step = jax.nn.softplus(step_raw + step_bias)
    keep = jnp.exp(-decay_rate * step)
    driven = step[:, :, None] * xs_heads
    new_state = keep[:, :, None, None] * scan_state + driven[:, :, :, None] * b_heads[:, :, None, :]
    read = jnp.sum(new_state * c_heads[:, :, None, :], axis=3).reshape(seqs, channels)
    gated = (read * jax.nn.silu(gate_z) * inner_gain.astype(jnp.float32)).astype(jnp.bfloat16)
    new_conv = history[:, :, 1:, :]
    whole_blocks = 2 * seqs * route_experts.shape[1] // expert_router.shape[1] >= seqs
    if whole_blocks and expert_gate.shape[0] == 1 and lax.axis_size("tp") == 4:
        layer_out = fused_tail(
            gated,
            proj_out,
            resid,
            post_gain,
            ffn_gain,
            group_router,
            expert_router,
            route_experts,
            expert_gate,
            expert_up,
            expert_down,
            dense_switch,
            dense_gate,
            dense_up,
            dense_down,
            out_gain,
        )
        return (layer_out, new_state, new_conv)
    mixed = lax.psum(
        jnp.dot(gated, proj_out, preferred_element_type=jnp.float32).astype(jnp.bfloat16), "tp"
    ).astype(jnp.float32)
    stream = (resid.astype(jnp.float32) + scaled_rows(mixed, post_gain)).astype(jnp.bfloat16)
    feed = scaled_rows(stream, ffn_gain).astype(jnp.bfloat16)
    feed_quarter = lax.dynamic_slice_in_dim(feed, tp_index * quarter, quarter, 1)
    expert_count = expert_router.shape[1]
    group_size = expert_count // group_router.shape[1]
    pick_count = route_experts.shape[1]
    group_prob = softmax_plain(jnp.dot(feed, group_router, preferred_element_type=jnp.float32))
    expert_logits = jnp.dot(feed, expert_router, preferred_element_type=jnp.float32)
    matches = route_experts[:, :, None] == jnp.arange(expert_count, dtype=jnp.int32)[None, None, :]
    pick_logits = jnp.sum(jnp.where(matches, expert_logits[:, None, :], 0.0), axis=2)
    chosen_group = route_experts[:, 0] // group_size
    group_ids = jnp.arange(group_router.shape[1], dtype=jnp.int32)
    group_weight = jnp.sum(
        jnp.where(chosen_group[:, None] == group_ids[None, :], group_prob, 0.0), axis=1
    )
    pick_weight = softmax_plain(pick_logits) * group_weight[:, None]
    capacity = 2 * seqs * pick_count // expert_count
    flat_picks = route_experts.reshape(-1)
    one_hot = (flat_picks[:, None] == jnp.arange(expert_count, dtype=jnp.int32)[None, :]).astype(
        jnp.int32
    )
    slot = jnp.sum((jnp.cumsum(one_hot, axis=0) - one_hot) * one_hot, axis=1)
    target = flat_picks * capacity + slot
    repeated = jnp.repeat(feed, pick_count, axis=0)
    outgoing = jnp.zeros((expert_count * capacity, width), jnp.bfloat16).at[target].set(repeated)
    outgoing = outgoing.reshape(expert_count, capacity, width)
    arrived = lax.all_to_all(outgoing, "ep", split_axis=0, concat_axis=0, tiled=True)
    sources = arrived.shape[0]
    items = arrived.shape[1]
    rows = arrived.reshape(sources * items, width)
    gate_value = jnp.dot(rows, expert_gate[0], preferred_element_type=jnp.float32)
    up_value = jnp.dot(rows, expert_up[0], preferred_element_type=jnp.float32)
    hidden = (jax.nn.silu(gate_value) * up_value).astype(jnp.bfloat16)
    result = jnp.dot(hidden, expert_down[0], preferred_element_type=jnp.float32).reshape(
        sources, items, width
    )
    summed = lax.psum_scatter(result.astype(jnp.bfloat16), "tp", scatter_dimension=2, tiled=True)
    returned = lax.all_to_all(summed, "ep", split_axis=0, concat_axis=0, tiled=True)
    fetched = returned.reshape(expert_count * capacity, quarter)[target].reshape(
        seqs, pick_count, quarter
    )
    routed = jnp.sum(fetched.astype(jnp.float32) * pick_weight[:, :, None], axis=1)
    gate_piece = jnp.einsum(
        "sd,cd->sc",
        feed_quarter,
        lax.all_gather(dense_gate, "ep", axis=0, tiled=True),
        preferred_element_type=jnp.float32,
    )
    up_piece = jnp.einsum(
        "sd,cd->sc",
        feed_quarter,
        lax.all_gather(dense_up, "ep", axis=0, tiled=True),
        preferred_element_type=jnp.float32,
    )
    gate_sum = gate_piece
    up_sum = up_piece
    gate_sum, up_sum = (
        lax.psum(gate_sum.astype(jnp.bfloat16), "tp").astype(jnp.float32),
        lax.psum(up_sum.astype(jnp.bfloat16), "tp").astype(jnp.float32),
    )
    dense_hidden = (jax.nn.silu(gate_sum) * up_sum).astype(jnp.bfloat16)
    dense_out = jnp.dot(
        dense_hidden,
        lax.all_gather(dense_down, "ep", axis=0, tiled=True),
        preferred_element_type=jnp.float32,
    )
    switch = jax.nn.sigmoid(jnp.dot(feed, dense_switch, preferred_element_type=jnp.float32))
    combined = routed + switch[:, None] * dense_out
    total_square = lax.psum(jnp.sum(combined * combined, axis=1), "tp")
    scale = lax.rsqrt(total_square / width + norm_eps)
    stream_part = lax.dynamic_slice_in_dim(stream, tp_index * quarter, quarter, 1).astype(
        jnp.float32
    )
    layer_out = (stream_part + combined * scale[:, None] * out_gain.astype(jnp.float32)).astype(
        jnp.bfloat16
    )
    return (layer_out, new_state, new_conv)


def solution(mesh):
    placed = (
        P("ep", None),
        P(),
        P(None, "tp"),
        P(None, "tp"),
        P(None, "tp"),
        P(None, "tp"),
        P(),
        P("tp"),
        P("tp"),
        P(None, None, "tp"),
        P("ep", None, None, "tp"),
        P("ep", "tp", None, None),
        P("tp"),
        P("tp", None),
        P(),
        P(),
        P(),
        P(),
        P("ep", None),
        P("ep", None, "tp"),
        P("ep", None, "tp"),
        P("ep", "tp", None),
        P(),
        P("ep", "tp"),
        P("ep", "tp"),
        P("ep", "tp"),
        P("tp"),
    )
    return jax.shard_map(
        on_device,
        mesh=mesh,
        in_specs=placed,
        out_specs=(P("ep", "tp"), P("ep", "tp", None, None), P("ep", None, None, "tp")),
        check_vma=False,
    )
```

```python
import functools

import jax
import jax.numpy as jnp
from jax import lax
from jax.experimental import pallas as pl
from jax.experimental.pallas import tpu as pltpu
from jax.sharding import PartitionSpec as P

norm_eps = 1e-06


def scaled_rows(values, gain):
    values = values.astype(jnp.float32)
    mean_square = jnp.mean(values * values, axis=-1, keepdims=True)
    return values * lax.rsqrt(mean_square + norm_eps) * gain.astype(jnp.float32)


def softmax_plain(logits):
    weights = jnp.exp(logits)
    return weights / jnp.sum(weights, axis=-1, keepdims=True)


def fused_kernel(
    ep,
    group_size,
    group_count,
    expert_count,
    proj_out_ref,
    resid_ref,
    mix_ref,
    post_ref,
    ffn_ref,
    expert_router_ref,
    group_router_ref,
    switch_ref,
    route_ref,
    out_gain_ref,
    inner_ref,
    proj_step_ref,
    taps_ref,
    conv_ref,
    bias_ref,
    decay_ref,
    proj_x_hbm,
    proj_z_hbm,
    proj_b_hbm,
    proj_c_hbm,
    state_hbm,
    gate_hbm,
    up_hbm,
    down_hbm,
    dense_gate_hbm,
    dense_up_hbm,
    dense_down_hbm,
    out_ref,
    new_state_hbm,
    new_conv_ref,
    proj_w,
    state_buf,
    new_state_buf,
    router_buf,
    gate_w,
    up_w,
    down_w,
    dgate,
    dup,
    ddown,
    stream_buf,
    mix_own,
    mix_peer,
    half_own,
    half_far,
    rows_buf,
    aux_buf,
    part_buf,
    part_peer,
    send_x,
    recv_x,
    send_ep,
    recv_ep,
    square_own,
    square_peer,
    local_sem,
    state_sem,
    dense_send,
    dense_recv,
    mix_send,
    mix_recv,
    rows_send,
    rows_recv,
    aux_send,
    aux_recv,
    forward_send,
    forward_recv,
    part_send,
    part_recv,
    x_send,
    x_recv,
    ep_send,
    ep_recv,
    square_send,
    square_recv,
):
    f32, bf16 = jnp.float32, jnp.bfloat16
    me = lax.axis_index("ep")
    tp = lax.axis_index("tp")
    far = tp // 2
    core = tp % 2
    beside = far * 2 + (1 - core)
    across = (1 - far) * 2 + core
    diagonal = (1 - far) * 2 + (1 - core)
    near = (beside, across, diagonal)
    seqs, width = resid_ref.shape
    quarter = width // 4
    share = dgate.shape[1]

    def remote(src, dst, send, recv, ep_to, tp_to):
        return pltpu.make_async_remote_copy(
            src_ref=src,
            dst_ref=dst,
            send_sem=send,
            recv_sem=recv,
            device_id=(ep_to, tp_to),
            device_id_type=pl.DeviceIdType.MESH,
        )

    def ep_at(step):
        return lax.rem(me + step + ep, ep)

    local = []

    def load(src, dst):
        copy = pltpu.make_async_copy(src, dst, local_sem.at[len(local)])
        copy.start()
        local.append(copy)

    for k, src in enumerate((proj_x_hbm, proj_b_hbm, proj_c_hbm, proj_z_hbm)):
        load(src, proj_w.at[k])
    load(state_hbm, state_buf)
    load(gate_hbm.at[0], gate_w)
    load(up_hbm.at[0], up_w)
    for q in range(4):
        load(down_hbm.at[0, :, pl.ds(q * quarter, quarter)], down_w.at[q])
    dense_pairs = ((dense_gate_hbm, dgate), (dense_up_hbm, dup), (dense_down_hbm, ddown))
    for src, dst in dense_pairs:
        load(src.at[pl.ds(tp * share, share), :], dst.at[tp])

    barrier = pltpu.get_barrier_semaphore()
    for step in range(1, ep):
        pl.semaphore_signal(
            barrier, inc=1, device_id=(ep_at(step), tp), device_id_type=pl.DeviceIdType.MESH
        )
    for peer in near:
        pl.semaphore_signal(
            barrier, inc=1, device_id=(me, peer), device_id_type=pl.DeviceIdType.MESH
        )

    def row(ref):
        return ref[...].astype(f32).reshape(1, ref.shape[0])

    resid_f = resid_ref[...].astype(f32)
    resid_scale = lax.rsqrt(jnp.mean(resid_f * resid_f, axis=1, keepdims=True) + norm_eps)
    normed = (resid_f * resid_scale * row(mix_ref)).astype(bf16)
    group_base = -(-expert_count // 8) * 8
    switch_lane = group_base + -(-group_count // 8) * 8
    router_buf[...] = jnp.zeros_like(router_buf)
    router_buf[0:expert_count, :] = expert_router_ref[...].astype(f32)
    router_buf[group_base : group_base + group_count, :] = group_router_ref[...].astype(f32)
    router_buf[switch_lane : switch_lane + 1, :] = row(switch_ref)
    nt = (((1,), (1,)), ((), ()))
    step_all = lax.dot_general(normed, proj_step_ref[...], nt, preferred_element_type=f32)
    pl.semaphore_wait(barrier, ep - 1 + 3)

    sends = []
    dense_copies = []
    for t, (src, dst) in enumerate(dense_pairs):
        for k, peer in enumerate(near):
            copy = remote(
                src.at[pl.ds(peer * share, share), :],
                dst.at[tp],
                dense_send.at[3 * t + k],
                dense_recv.at[3 * t + k],
                me,
                peer,
            )
            copy.start()
            dense_copies.append(copy)
    sends += dense_copies

    channels = conv_ref.shape[3]
    heads = bias_ref.shape[0]
    head_dim = channels // heads
    taps = taps_ref[...].astype(f32)
    old = conv_ref.shape[1]
    active = []
    for k in range(3):
        local[k].wait()
        fresh = jnp.dot(normed, proj_w[k], preferred_element_type=f32).astype(bf16)
        summed = conv_ref[k, 0].astype(f32) * taps[k, 0:1]
        for tap in range(1, old):
            earlier = conv_ref[k, tap]
            new_conv_ref[k, tap - 1] = earlier
            summed = summed + earlier.astype(f32) * taps[k, tap : tap + 1]
        new_conv_ref[k, old - 1] = fresh
        summed = summed + fresh.astype(f32) * taps[k, old : old + 1]
        active.append(summed * jax.nn.sigmoid(summed))
    inputs, vec_in, vec_read = active
    local[3].wait()
    gate_z = jnp.dot(normed, proj_w[3], preferred_element_type=f32)
    step_lane = lax.broadcasted_iota(jnp.int32, step_all.shape, 1)
    lane_in = lax.broadcasted_iota(jnp.int32, (seqs, channels), 1)
    keep = jnp.zeros((seqs, channels), f32)
    stepped = jnp.zeros((seqs, channels), f32)
    for h in range(heads):
        raw = jnp.sum(
            jnp.where(step_lane == tp * heads + h, step_all, 0.0), axis=1, keepdims=True
        )
        raw = raw + bias_ref[h]
        step = jnp.maximum(raw, 0.0) + jnp.log1p(jnp.exp(-jnp.abs(raw)))
        mine = (lane_in >= h * head_dim) & (lane_in < (h + 1) * head_dim)
        keep = jnp.where(mine, jnp.exp(-decay_ref[h] * step), keep)
        stepped = jnp.where(mine, step, stepped)
    columns = jnp.concatenate(
        [keep, stepped * inputs, jnp.zeros((channels - 2 * seqs, channels), f32)], axis=0
    ).T
    local[4].wait()
    read_lane = lax.broadcasted_iota(jnp.int32, (channels, channels), 1)
    read = jnp.zeros((channels, channels), f32)
    for t in range(seqs):
        fresh_state = (
            columns[:, t : t + 1] * state_buf[t]
            + columns[:, seqs + t : seqs + t + 1] * vec_in[t : t + 1]
        )
        new_state_buf[t] = fresh_state
        value = jnp.sum(fresh_state * vec_read[t : t + 1], axis=1, keepdims=True)
        read = jnp.where(read_lane == t, value, read)
    read = read.T[0:seqs]
    gated = (read * (gate_z * jax.nn.sigmoid(gate_z)) * row(inner_ref)).astype(bf16)
    mix_own[...] = jnp.dot(gated, proj_out_ref[...], preferred_element_type=f32).astype(bf16)

    first = remote(mix_own, mix_peer, mix_send.at[0], mix_recv.at[0], me, beside)
    first.start()
    sends.append(first)
    first.wait_recv()
    half = width // 2
    chip_sum = (mix_own[...].astype(f32) + mix_peer[...].astype(f32)).astype(bf16)
    half_own[0] = chip_sum[:, :half]
    half_own[1] = chip_sum[:, half:]
    halves = []
    for k, peer in enumerate((across, diagonal)):
        copy = remote(
            half_own.at[core],
            half_far.at[core],
            mix_send.at[1 + k],
            mix_recv.at[1 + k],
            me,
            peer,
        )
        copy.start()
        halves.append(copy)
    sends += halves

    state_out = pltpu.make_async_copy(new_state_buf, new_state_hbm, state_sem)
    state_out.start()
    for copy in halves:
        copy.wait_recv()

    far_sum = jnp.concatenate([half_far[0], half_far[1]], axis=1)
    mixed = chip_sum.astype(f32) + far_sum.astype(f32)
    mixed_scale = lax.rsqrt(jnp.mean(mixed * mixed, axis=1, keepdims=True) + norm_eps)
    stream = (
        resid_f + mixed * mixed_scale * row(post_ref)
    ).astype(bf16)
    stream_f = stream.astype(f32)
    feed_scale = lax.rsqrt(jnp.mean(stream_f * stream_f, axis=1, keepdims=True) + norm_eps)
    feed = (stream_f * feed_scale * row(ffn_ref)).astype(bf16)
    for q in range(4):
        rows_buf[q, 0] = feed[:, q * quarter : (q + 1) * quarter]
        stream_buf[q] = stream[:, q * quarter : (q + 1) * quarter]

    rows_copies = []
    for step in range(1, ep):
        copy = remote(
            rows_buf.at[tp, 0],
            rows_buf.at[tp, step],
            rows_send.at[step],
            rows_recv.at[step],
            ep_at(step),
            tp,
        )
        copy.start()
        rows_copies.append(copy)
    sends += rows_copies

    logits = lax.dot_general(
        feed, router_buf[...].astype(bf16), nt, preferred_element_type=f32
    )
    lane = lax.broadcasted_iota(jnp.int32, logits.shape, 1)
    same = lax.broadcasted_iota(jnp.int32, (seqs, seqs), 0) == lax.broadcasted_iota(
        jnp.int32, (seqs, seqs), 1
    )
    route = lax.dot_general(
        jnp.where(same, 1.0, 0.0).astype(bf16),
        route_ref[...].astype(f32).astype(bf16),
        nt,
        preferred_element_type=f32,
    ).astype(jnp.int32)
    picked = lane == route[:, 0:1]
    for k in range(1, route.shape[1]):
        picked = picked | (lane == route[:, k : k + 1])
    weights = jnp.exp(logits)
    pick = jnp.where(picked, weights, 0.0)
    group_lane = (lane - group_base) * group_size
    in_groups = (lane >= group_base) & (lane < group_base + group_count)
    group = jnp.where(in_groups, weights, 0.0)
    lead = route[:, 0:1]
    chosen = in_groups & (lead >= group_lane) & (lead < group_lane + group_size)
    group_weight = jnp.sum(jnp.where(chosen, weights, 0.0), axis=1, keepdims=True) / jnp.sum(
        group, axis=1, keepdims=True
    )
    pick = pick / jnp.sum(pick, axis=1, keepdims=True) * group_weight
    aux_buf[0] = jnp.where(lane == switch_lane, jax.nn.sigmoid(logits), pick).astype(bf16)
    aux_copies = []
    for step in range(1, ep):
        copy = remote(
            aux_buf.at[0],
            aux_buf.at[step],
            aux_send.at[step],
            aux_recv.at[step],
            ep_at(step),
            tp,
        )
        copy.start()
        aux_copies.append(copy)
    sends += aux_copies

    to_beside, to_across, to_last = [], [], []
    for step in range(1, ep):
        rows_copies[step - 1].wait_recv()
        for k, (peer, kept) in enumerate(((across, to_across), (beside, to_beside))):
            copy = remote(
                rows_buf.at[tp, step],
                rows_buf.at[tp, step],
                forward_send.at[k, step],
                forward_recv.at[k, step],
                me,
                peer,
            )
            copy.start()
            kept.append(copy)
    for step in range(1, ep):
        to_across[step - 1].wait_recv()
        copy = remote(
            rows_buf.at[across, step],
            rows_buf.at[across, step],
            forward_send.at[2, step],
            forward_recv.at[2, step],
            me,
            beside,
        )
        copy.start()
        to_last.append(copy)
    sends += to_across + to_beside + to_last
    for copy in local[5:]:
        copy.wait()
    for copy in dense_copies + aux_copies + to_beside + to_last:
        copy.wait_recv()

    total = ep * seqs
    gate = up = dense_g = dense_u = None

    def add(total_sum, value):
        return value if total_sum is None else total_sum + value

    for q in range(4):
        rows = rows_buf[q].reshape(total, quarter)
        span = pl.ds(q * quarter, quarter)
        gate = add(gate, jnp.dot(rows, gate_w[span, :], preferred_element_type=f32))
        up = add(up, jnp.dot(rows, up_w[span, :], preferred_element_type=f32))
        dense_g = add(dense_g, lax.dot_general(rows, dgate[q], nt, preferred_element_type=f32))
        dense_u = add(dense_u, lax.dot_general(rows, dup[q], nt, preferred_element_type=f32))
    aux = aux_buf[...].reshape(total, aux_buf.shape[2]).astype(f32)
    aux_lane = lax.broadcasted_iota(jnp.int32, aux.shape, 1)
    weight = jnp.sum(jnp.where(aux_lane == me, aux, 0.0), axis=1, keepdims=True)
    switch = jnp.sum(jnp.where(aux_lane == switch_lane, aux, 0.0), axis=1, keepdims=True)
    hidden = (gate * jax.nn.sigmoid(gate) * up * weight).astype(bf16)
    dense_hidden = (dense_g * jax.nn.sigmoid(dense_g) * dense_u * switch).astype(bf16)

    part_copies = []
    for k, q in enumerate((diagonal, beside, across, tp)):
        value = jnp.dot(hidden, down_w[q], preferred_element_type=f32) + jnp.dot(
            dense_hidden, ddown[q], preferred_element_type=f32
        )
        part_buf[q] = value.astype(bf16).reshape(ep, seqs, quarter)
        if k < 2:
            copy = remote(
                part_buf.at[q], part_peer.at[k], part_send.at[k], part_recv.at[k], me, beside
            )
            copy.start()
            part_copies.append(copy)
    sends += part_copies

    order = list(range(1, ep)) + [0]
    part_copies[0].wait_recv()
    x_copies = {}
    for step in order:
        send_x[step] = (
            part_buf[across, step].astype(f32) + part_peer[0, step].astype(f32)
        ).astype(bf16)
        copy = remote(
            send_x.at[step], recv_x.at[step], x_send.at[step], x_recv.at[step], me, across
        )
        copy.start()
        x_copies[step] = copy
        sends.append(copy)
    part_copies[1].wait_recv()
    combined = None
    ep_copies = []
    for step in order:
        x_copies[step].wait_recv()
        value = (
            part_buf[tp, step].astype(f32)
            + part_peer[1, step].astype(f32)
            + recv_x[step].astype(f32)
        )
        if step == 0:
            combined = value
            continue
        send_ep[step] = value.astype(bf16)
        copy = remote(
            send_ep.at[step],
            recv_ep.at[step],
            ep_send.at[step],
            ep_recv.at[step],
            ep_at(-step),
            tp,
        )
        copy.start()
        ep_copies.append(copy)
    sends += ep_copies
    for step in range(1, ep):
        ep_copies[step - 1].wait_recv()
        combined = combined + recv_ep[step].astype(f32)

    square = jnp.sum(combined * combined, axis=1, keepdims=True)
    square_own[...] = jnp.broadcast_to(square, square_own.shape)
    square_copies = []
    for k, peer in enumerate(near):
        copy = remote(
            square_own, square_peer.at[k], square_send.at[k], square_recv.at[k], me, peer
        )
        copy.start()
        square_copies.append(copy)
    sends += square_copies
    for copy in square_copies:
        copy.wait_recv()
    everything = (square_own[...] + square_peer[0]) + (square_peer[1] + square_peer[2])
    scale = lax.rsqrt(everything[:, 0:1] / width + norm_eps)
    own_stream = stream_buf[tp].astype(f32)
    out_ref[...] = (own_stream + combined * scale * row(out_gain_ref)).astype(bf16)
    state_out.wait()
    for copy in sends:
        copy.wait_send()


def fused_layer(
    resid,
    mix_gain,
    proj_x,
    proj_z,
    proj_b,
    proj_c,
    proj_step,
    step_bias,
    decay_rate,
    conv_taps,
    conv_state,
    scan_state,
    inner_gain,
    proj_out,
    post_gain,
    ffn_gain,
    group_router,
    expert_router,
    route_experts,
    expert_gate,
    expert_up,
    expert_down,
    dense_switch,
    dense_gate,
    dense_up,
    dense_down,
    out_gain,
):
    ep = lax.axis_size("ep")
    seqs, width = resid.shape
    quarter = width // 4
    channels = conv_state.shape[3]
    expert_count = expert_router.shape[1]
    group_count = group_router.shape[1]
    lanes = 128
    hidden_here = expert_gate.shape[2]
    share = dense_gate.shape[0] // 4
    bf16 = jnp.bfloat16
    vmem = pl.BlockSpec(memory_space=pltpu.VMEM)
    hbm = pl.BlockSpec(memory_space=pl.ANY)
    dma = pltpu.SemaphoreType.DMA
    kernel = functools.partial(
        fused_kernel, ep, expert_count // group_count, group_count, expert_count
    )
    smem = pl.BlockSpec(memory_space=pltpu.SMEM)
    earlier = conv_state.transpose(1, 2, 0, 3)
    state = scan_state.reshape(seqs, channels, scan_state.shape[3])
    layer_out, new_state, new_conv = pl.pallas_call(
        kernel,
        out_shape=(
            jax.ShapeDtypeStruct((seqs, quarter), bf16),
            jax.ShapeDtypeStruct(state.shape, state.dtype),
            jax.ShapeDtypeStruct(earlier.shape, earlier.dtype),
        ),
        in_specs=[vmem] * 14 + [smem] * 2 + [hbm] * 11,
        out_specs=(vmem, hbm, vmem),
        scratch_shapes=[
            pltpu.VMEM((4,) + proj_x.shape, bf16),
            pltpu.VMEM(state.shape, state.dtype),
            pltpu.VMEM(state.shape, state.dtype),
            pltpu.VMEM((lanes, width), jnp.float32),
            pltpu.VMEM((width, hidden_here), bf16),
            pltpu.VMEM((width, hidden_here), bf16),
            pltpu.VMEM((4, hidden_here, quarter), bf16),
            pltpu.VMEM((4, share, quarter), bf16),
            pltpu.VMEM((4, share, quarter), bf16),
            pltpu.VMEM((4, share, quarter), bf16),
            pltpu.VMEM((4, seqs, quarter), bf16),
            pltpu.VMEM((seqs, width), bf16),
            pltpu.VMEM((seqs, width), bf16),
            pltpu.VMEM((2, seqs, width // 2), bf16),
            pltpu.VMEM((2, seqs, width // 2), bf16),
            pltpu.VMEM((4, ep, seqs, quarter), bf16),
            pltpu.VMEM((ep, seqs, lanes), bf16),
            pltpu.VMEM((4, ep, seqs, quarter), bf16),
            pltpu.VMEM((2, ep, seqs, quarter), bf16),
            pltpu.VMEM((ep, seqs, quarter), bf16),
            pltpu.VMEM((ep, seqs, quarter), bf16),
            pltpu.VMEM((ep, seqs, quarter), bf16),
            pltpu.VMEM((ep, seqs, quarter), bf16),
            pltpu.VMEM((seqs, 128), jnp.float32),
            pltpu.VMEM((3, seqs, 128), jnp.float32),
            dma((14,)),
            dma,
            dma((9,)),
            dma((9,)),
            dma((3,)),
            dma((3,)),
            dma((ep,)),
            dma((ep,)),
            dma((ep,)),
            dma((ep,)),
            dma((3, ep)),
            dma((3, ep)),
            dma((2,)),
            dma((2,)),
            dma((ep,)),
            dma((ep,)),
            dma((ep,)),
            dma((ep,)),
            dma((3,)),
            dma((3,)),
        ],
        compiler_params=pltpu.CompilerParams(collective_id=0, has_side_effects=True),
        name="fused_layer",
    )(
        proj_out,
        resid,
        mix_gain,
        post_gain,
        ffn_gain,
        expert_router.T,
        group_router.T,
        dense_switch,
        route_experts.T,
        out_gain,
        inner_gain,
        proj_step.T,
        conv_taps,
        earlier,
        step_bias,
        decay_rate,
        proj_x,
        proj_z,
        proj_b,
        proj_c,
        state,
        expert_gate,
        expert_up,
        expert_down,
        dense_gate,
        dense_up,
        dense_down,
    )
    return layer_out, new_state.reshape(scan_state.shape), new_conv.transpose(2, 0, 1, 3)


def on_device(
    resid,
    mix_gain,
    proj_x,
    proj_z,
    proj_b,
    proj_c,
    proj_step,
    step_bias,
    decay_rate,
    conv_taps,
    conv_state,
    scan_state,
    inner_gain,
    proj_out,
    post_gain,
    ffn_gain,
    group_router,
    expert_router,
    route_experts,
    expert_gate,
    expert_up,
    expert_down,
    dense_switch,
    dense_gate,
    dense_up,
    dense_down,
    out_gain,
):
    tp_index = lax.axis_index("tp")
    seqs = resid.shape[0]
    width = resid.shape[1]
    quarter = width // lax.axis_size("tp")
    heads_here = scan_state.shape[1]
    head_dim = scan_state.shape[2]
    state_dim = scan_state.shape[3]
    channels = conv_state.shape[3]
    repeat = heads_here // (channels // state_dim)
    whole_blocks = 2 * seqs * route_experts.shape[1] // expert_router.shape[1] >= seqs
    one_group = channels == state_dim == 128 and expert_router.shape[1] <= 64
    few = lax.axis_size("tp") == 4 and expert_gate.shape[0] == 1
    if whole_blocks and one_group and few:
        return fused_layer(
            resid,
            mix_gain,
            proj_x,
            proj_z,
            proj_b,
            proj_c,
            proj_step,
            step_bias,
            decay_rate,
            conv_taps,
            conv_state,
            scan_state,
            inner_gain,
            proj_out,
            post_gain,
            ffn_gain,
            group_router,
            expert_router,
            route_experts,
            expert_gate,
            expert_up,
            expert_down,
            dense_switch,
            dense_gate,
            dense_up,
            dense_down,
            out_gain,
        )
    normed = scaled_rows(resid, mix_gain).astype(jnp.bfloat16)
    fresh = jnp.stack(
        [
            jnp.dot(normed, proj_x, preferred_element_type=jnp.float32),
            jnp.dot(normed, proj_b, preferred_element_type=jnp.float32),
            jnp.dot(normed, proj_c, preferred_element_type=jnp.float32),
        ],
        axis=1,
    ).astype(jnp.bfloat16)
    gate_z = jnp.dot(normed, proj_z, preferred_element_type=jnp.float32)
    step_all = jnp.dot(normed, proj_step, preferred_element_type=jnp.float32)
    step_raw = lax.dynamic_slice_in_dim(step_all, tp_index * heads_here, heads_here, 1)
    history = jnp.concatenate([conv_state, fresh[:, :, None, :]], axis=2)
    activated = jax.nn.silu(
        jnp.sum(history.astype(jnp.float32) * conv_taps.astype(jnp.float32)[None], axis=2)
    )
    xs_heads = activated[:, 0].reshape(seqs, heads_here, head_dim)
    b_heads = jnp.repeat(activated[:, 1].reshape(seqs, -1, state_dim), repeat, axis=1)
    c_heads = jnp.repeat(activated[:, 2].reshape(seqs, -1, state_dim), repeat, axis=1)
    step = jax.nn.softplus(step_raw + step_bias)
    keep = jnp.exp(-decay_rate * step)
    driven = step[:, :, None] * xs_heads
    new_state = keep[:, :, None, None] * scan_state + driven[:, :, :, None] * b_heads[:, :, None, :]
    read = jnp.sum(new_state * c_heads[:, :, None, :], axis=3).reshape(seqs, channels)
    gated = (read * jax.nn.silu(gate_z) * inner_gain.astype(jnp.float32)).astype(jnp.bfloat16)
    new_conv = history[:, :, 1:, :]
    mixed = lax.psum(
        jnp.dot(gated, proj_out, preferred_element_type=jnp.float32).astype(jnp.bfloat16), "tp"
    ).astype(jnp.float32)
    stream = (resid.astype(jnp.float32) + scaled_rows(mixed, post_gain)).astype(jnp.bfloat16)
    feed = scaled_rows(stream, ffn_gain).astype(jnp.bfloat16)
    feed_quarter = lax.dynamic_slice_in_dim(feed, tp_index * quarter, quarter, 1)
    expert_count = expert_router.shape[1]
    group_size = expert_count // group_router.shape[1]
    pick_count = route_experts.shape[1]
    group_prob = softmax_plain(jnp.dot(feed, group_router, preferred_element_type=jnp.float32))
    expert_logits = jnp.dot(feed, expert_router, preferred_element_type=jnp.float32)
    matches = route_experts[:, :, None] == jnp.arange(expert_count, dtype=jnp.int32)[None, None, :]
    pick_logits = jnp.sum(jnp.where(matches, expert_logits[:, None, :], 0.0), axis=2)
    chosen_group = route_experts[:, 0] // group_size
    group_ids = jnp.arange(group_router.shape[1], dtype=jnp.int32)
    group_weight = jnp.sum(
        jnp.where(chosen_group[:, None] == group_ids[None, :], group_prob, 0.0), axis=1
    )
    pick_weight = softmax_plain(pick_logits) * group_weight[:, None]
    capacity = 2 * seqs * pick_count // expert_count
    flat_picks = route_experts.reshape(-1)
    one_hot = (flat_picks[:, None] == jnp.arange(expert_count, dtype=jnp.int32)[None, :]).astype(
        jnp.int32
    )
    slot = jnp.sum((jnp.cumsum(one_hot, axis=0) - one_hot) * one_hot, axis=1)
    target = flat_picks * capacity + slot
    repeated = jnp.repeat(feed, pick_count, axis=0)
    outgoing = jnp.zeros((expert_count * capacity, width), jnp.bfloat16).at[target].set(repeated)
    outgoing = outgoing.reshape(expert_count, capacity, width)
    arrived = lax.all_to_all(outgoing, "ep", split_axis=0, concat_axis=0, tiled=True)
    sources = arrived.shape[0]
    items = arrived.shape[1]
    rows = arrived.reshape(sources * items, width)
    gate_value = jnp.dot(rows, expert_gate[0], preferred_element_type=jnp.float32)
    up_value = jnp.dot(rows, expert_up[0], preferred_element_type=jnp.float32)
    hidden = (jax.nn.silu(gate_value) * up_value).astype(jnp.bfloat16)
    result = jnp.dot(hidden, expert_down[0], preferred_element_type=jnp.float32).reshape(
        sources, items, width
    )
    summed = lax.psum_scatter(result.astype(jnp.bfloat16), "tp", scatter_dimension=2, tiled=True)
    returned = lax.all_to_all(summed, "ep", split_axis=0, concat_axis=0, tiled=True)
    fetched = returned.reshape(expert_count * capacity, quarter)[target].reshape(
        seqs, pick_count, quarter
    )
    routed = jnp.sum(fetched.astype(jnp.float32) * pick_weight[:, :, None], axis=1)
    gate_piece = jnp.einsum(
        "sd,cd->sc",
        feed_quarter,
        lax.all_gather(dense_gate, "ep", axis=0, tiled=True),
        preferred_element_type=jnp.float32,
    )
    up_piece = jnp.einsum(
        "sd,cd->sc",
        feed_quarter,
        lax.all_gather(dense_up, "ep", axis=0, tiled=True),
        preferred_element_type=jnp.float32,
    )
    gate_sum = gate_piece
    up_sum = up_piece
    gate_sum, up_sum = (
        lax.psum(gate_sum.astype(jnp.bfloat16), "tp").astype(jnp.float32),
        lax.psum(up_sum.astype(jnp.bfloat16), "tp").astype(jnp.float32),
    )
    dense_hidden = (jax.nn.silu(gate_sum) * up_sum).astype(jnp.bfloat16)
    dense_out = jnp.dot(
        dense_hidden,
        lax.all_gather(dense_down, "ep", axis=0, tiled=True),
        preferred_element_type=jnp.float32,
    )
    switch = jax.nn.sigmoid(jnp.dot(feed, dense_switch, preferred_element_type=jnp.float32))
    combined = routed + switch[:, None] * dense_out
    total_square = lax.psum(jnp.sum(combined * combined, axis=1), "tp")
    scale = lax.rsqrt(total_square / width + norm_eps)
    stream_part = lax.dynamic_slice_in_dim(stream, tp_index * quarter, quarter, 1).astype(
        jnp.float32
    )
    layer_out = (stream_part + combined * scale[:, None] * out_gain.astype(jnp.float32)).astype(
        jnp.bfloat16
    )
    return (layer_out, new_state, new_conv)


def solution(mesh):
    placed = (
        P("ep", None),
        P(),
        P(None, "tp"),
        P(None, "tp"),
        P(None, "tp"),
        P(None, "tp"),
        P(),
        P("tp"),
        P("tp"),
        P(None, None, "tp"),
        P("ep", None, None, "tp"),
        P("ep", "tp", None, None),
        P("tp"),
        P("tp", None),
        P(),
        P(),
        P(),
        P(),
        P("ep", None),
        P("ep", None, "tp"),
        P("ep", None, "tp"),
        P("ep", "tp", None),
        P(),
        P("ep", "tp"),
        P("ep", "tp"),
        P("ep", "tp"),
        P("tp"),
    )
    return jax.shard_map(
        on_device,
        mesh=mesh,
        in_specs=placed,
        out_specs=(P("ep", "tp"), P("ep", "tp", None, None), P("ep", None, None, "tp")),
        check_vma=False,
    )
```
